32 devices in a mesh: sp: 8 (over z, y), tp: 4 (over x, core).
Axes of the slice: x: 2, y: 2, z: 4, core: 2. Of those that a mesh axis runs over, the one named last changes fastest.
Arguments:
- residual_input_stream: bfloat16 [8192, 2048], P(('sp', 'tp')), may hold values from -6 to 6
- receptance: bfloat16 [8192, 1024], P('sp', 'tp'), may hold values from -6 to 6
- key_matrix_all: bfloat16 [8192, 1024], P('sp', 'tp'), may hold values from -6 to 6
- value_matrix_all: bfloat16 [8192, 1024], P('sp', 'tp'), may hold values from -6 to 6
- decay_preactivation: bfloat16 [8192, 1024], P('sp', 'tp'), may hold values from -15 to 1
- learning_rate_preactivation: bfloat16 [8192, 1024], P('sp', 'tp'), may hold values from -11 to 5
- output_gate_all_heads: bfloat16 [8192, 1024], P('sp', 'tp'), may hold values from -6 to 6
- extra_log_decay: float32 [8192, 1024], P('sp', 'tp'), may hold values from -0.7 to 0
- head_norm_gain: float32 [1024], P('tp'), may hold values from 0.1 to 1.9
- output_projection_weight: bfloat16 [1024, 2048], P('tp'), may hold values from -0.1875 to 0.1875
- feedforward_norm_gain: float32 [2048], replicated, may hold values from 0.1 to 1.9
- gate_projection_weight: bfloat16 [2048, 5632], P('sp', 'tp'), may hold values from -0.125 to 0.125
- up_projection_weight: bfloat16 [2048, 5632], P('sp', 'tp'), may hold values from -0.125 to 0.125
- down_projection_weight: bfloat16 [2048, 5632], P('sp', 'tp'), may hold values from -0.078125 to 0.078125
- convolution_kernel: bfloat16 [3, 2, 5632], P(None, None, 'tp'), may hold values from -3.5 to 3.5
Outputs:
- layer_out: bfloat16 [8192, 2048], P(('sp', 'tp'))
The draws below stay inside these ranges and needn't reach their ends.
All inputs are finite; a program needn't handle non-finite values.
Results may differ from the reference program's by a relative error of at most 0.022.
Values may be sent and summed in bfloat16 or wider, within the bound.
A program may use at most 128 MiB of HBM per device.

```python
import math
import jax
import jax.numpy as jnp
from jax import lax

D = 2048
HEAD_TOTAL = 16
HEAD_WIDTH = 64
FF = 5632
TOK_DEV = 1024
TOKEN_TOTAL = 8192
N_TP = 4


def slow_heads(key):
    share = 0.5
    return jax.random.uniform(jax.random.fold_in(key, 7), (HEAD_TOTAL,)) < share


def head_noise(key, scale):
    return scale * jax.random.truncated_normal(key, -4.0, 4.0, (TOKEN_TOTAL, HEAD_TOTAL * HEAD_WIDTH), jnp.float32)


def draw_decay_preactivation(key, part):
    slow = slow_heads(key)
    base = jnp.repeat(jnp.where(slow, -10.5, -3.2), HEAD_WIDTH)
    noise = head_noise(jax.random.fold_in(key, 1), 0.8)
    offsets = jax.random.uniform(jax.random.fold_in(key, 2), (TOKEN_TOTAL // TOK_DEV, 1), jnp.float32, -0.8, 0.8)
    return (base[None, :] + noise + jnp.repeat(offsets, TOK_DEV, axis=0)).astype(jnp.bfloat16)


def draw_learning_rate_preactivation(key, part):
    slow = slow_heads(key)
    base = jnp.repeat(jnp.where(slow, -6.5, 0.5), HEAD_WIDTH)
    noise = head_noise(jax.random.fold_in(key, 3), 1.0)
    return (base[None, :] + noise).astype(jnp.bfloat16)


def draw_extra_log_decay(key, part):
    hits = jax.random.uniform(jax.random.fold_in(key, 4), (TOKEN_TOTAL, HEAD_TOTAL)) < 4.0 / TOKEN_TOTAL
    values = jax.random.uniform(jax.random.fold_in(key, 5), (TOKEN_TOTAL, HEAD_TOTAL * HEAD_WIDTH), jnp.float32, math.log(0.5), math.log(0.8))
    return jnp.where(jnp.repeat(hits, HEAD_WIDTH, axis=1), values, 0.0)


def level_of(own_key, shape, shards, least, high):
    def one(axis_at, parts):
        draws = jax.random.uniform(jax.random.fold_in(jax.random.fold_in(own_key, 6), axis_at), (parts,), jnp.float32, least / len(shards), high / len(shards))
        return jnp.repeat(jnp.exp(draws), shape[axis_at] // parts).reshape((-1,) + (1,) * (len(shape) - axis_at - 1))

    level = one(*shards[0])
    for cut in shards[1:]:
        level = level * one(*cut)
    return level


def scatter_about(key, shape, scale, bound, shards=(), dtype=jnp.bfloat16):
    array = scale * jax.random.normal(key, shape, jnp.float32)
    if shards:
        array = array * level_of(key, shape, shards, -0.22, 0.18)
    return jnp.clip(array, -bound, bound).astype(dtype)


def setup_inputs(seed: int = 0) -> dict:
    streams_of = jax.random.split(jax.random.key(seed), 16)
    return {
        "residual_input_stream": scatter_about(streams_of[0], (TOKEN_TOTAL, D), 1.0, 6.0, ((0, 32),)),
        "receptance": scatter_about(streams_of[1], (TOKEN_TOTAL, HEAD_TOTAL * HEAD_WIDTH), 1.0, 6.0, ((0, 8), (1, 4))),
        "key_matrix_all": scatter_about(streams_of[2], (TOKEN_TOTAL, HEAD_TOTAL * HEAD_WIDTH), 1.0, 6.0, ((0, 8), (1, 4))),
        "value_matrix_all": scatter_about(streams_of[3], (TOKEN_TOTAL, HEAD_TOTAL * HEAD_WIDTH), 1.0, 6.0, ((0, 8), (1, 4))),
        "decay_preactivation": draw_decay_preactivation(jax.random.fold_in(streams_of[15], 71), 0),
        "learning_rate_preactivation": draw_learning_rate_preactivation(jax.random.fold_in(streams_of[15], 71), 0),
        "output_gate_all_heads": scatter_about(streams_of[6], (TOKEN_TOTAL, HEAD_TOTAL * HEAD_WIDTH), 1.0, 6.0, ((0, 8), (1, 4))),
        "extra_log_decay": draw_extra_log_decay(jax.random.fold_in(streams_of[15], 71), 0),
        "head_norm_gain": jnp.clip(1.0 + 0.18 * jax.random.normal(streams_of[8], (HEAD_TOTAL * HEAD_WIDTH,), jnp.float32), 0.1, 1.9),
        "output_projection_weight": scatter_about(streams_of[9], (HEAD_TOTAL * HEAD_WIDTH, D), (HEAD_TOTAL * HEAD_WIDTH) ** -0.5, 0.1875, ((0, 4),)),
        "feedforward_norm_gain": jnp.clip(1.0 + 0.18 * jax.random.normal(streams_of[10], (D,), jnp.float32), 0.1, 1.9),
        "gate_projection_weight": scatter_about(streams_of[11], (D, FF), D ** -0.5, 0.125, ((0, 8), (1, 4))),
        "up_projection_weight": scatter_about(streams_of[12], (D, FF), D ** -0.5, 0.125, ((0, 8), (1, 4))),
        "down_projection_weight": scatter_about(streams_of[13], (D, FF), FF ** -0.5, 0.078125, ((0, 8), (1, 4))),
        "convolution_kernel": scatter_about(streams_of[14], (3, 2, FF), 0.577, 3.5, ((2, 4),)),
    }


highest = lax.Precision.HIGHEST

def per_head_layout(values_in):
    return values_in.astype(jnp.float32).reshape(values_in.shape[0], HEAD_TOTAL, HEAD_WIDTH)

def reference(residual_input_stream, receptance, key_matrix_all, value_matrix_all, decay_preactivation, learning_rate_preactivation, output_gate_all_heads, extra_log_decay, head_norm_gain, output_projection_weight, feedforward_norm_gain, gate_projection_weight, up_projection_weight, down_projection_weight, convolution_kernel):
    queries = per_head_layout(receptance)
    keys = per_head_layout(key_matrix_all)
    values = per_head_layout(value_matrix_all)
    decay_logarithm = -jnp.exp(-jax.nn.softplus(-per_head_layout(decay_preactivation)) - 0.5) + extra_log_decay.reshape(TOKEN_TOTAL, HEAD_TOTAL, HEAD_WIDTH)
    factors = jnp.exp(decay_logarithm)
    rates = jax.nn.sigmoid(per_head_layout(learning_rate_preactivation))
    normed_keys = keys * lax.rsqrt(lax.optimization_barrier(jnp.sum(keys * keys, axis=-1, keepdims=True)) + 1e-06)
    removal = normed_keys * rates

    def advance(carried, inputs_now):
        query_now, key_now, value_now, factor_now, normed_now, removal_now = inputs_now
        along = jnp.einsum('hvk,hk->hv', carried, normed_now, precision=highest)
        carried = carried * factor_now[:, None, :] - along[:, :, None] * removal_now[:, None, :] + value_now[:, :, None] * key_now[:, None, :]
        return (carried, jnp.einsum('hvk,hk->hv', carried, query_now, precision=highest))
    start_state = jnp.zeros((HEAD_TOTAL, HEAD_WIDTH, HEAD_WIDTH), jnp.float32)
    final_state, readout = lax.scan(advance, start_state, (queries, keys, values, factors, normed_keys, removal))
    centered = readout - lax.optimization_barrier(jnp.mean(readout, axis=-1, keepdims=True))
    variance = lax.optimization_barrier(jnp.mean(centered * centered, axis=-1, keepdims=True))
    normalized = (centered * lax.rsqrt(variance + 0.00064)).reshape(TOKEN_TOTAL, HEAD_TOTAL * HEAD_WIDTH)
    mixed_out = (normalized * head_norm_gain * output_gate_all_heads.astype(jnp.float32)).astype(jnp.bfloat16)
    group_width = HEAD_TOTAL * HEAD_WIDTH // N_TP
    attention = jnp.zeros((TOKEN_TOTAL, D), jnp.float32)
    for group in range(N_TP):
        part = jnp.dot(mixed_out[:, group * group_width:(group + 1) * group_width], output_projection_weight[group * group_width:(group + 1) * group_width], preferred_element_type=jnp.float32)
        attention = attention + lax.optimization_barrier(part.astype(jnp.bfloat16)).astype(jnp.float32)
    stream = lax.optimization_barrier((residual_input_stream.astype(jnp.float32) + attention).astype(jnp.bfloat16))
    stream_wide = stream.astype(jnp.float32)
    normed = (stream_wide * lax.rsqrt(lax.optimization_barrier(jnp.mean(stream_wide * stream_wide, axis=-1, keepdims=True)) + 1e-06) * feedforward_norm_gain).astype(jnp.bfloat16)
    taps = convolution_kernel.astype(jnp.float32)
    unit_width = FF // N_TP
    block_count = TOKEN_TOTAL // TOK_DEV

    def ffn_block(carried, inputs_now):
        normed_block, stream_block = inputs_now
        gate_pre = jnp.dot(normed_block, gate_projection_weight, preferred_element_type=jnp.float32).astype(jnp.bfloat16)
        up_pre = jnp.dot(normed_block, up_projection_weight, preferred_element_type=jnp.float32).astype(jnp.bfloat16)
        gate_ext = jnp.concatenate([carried[0], gate_pre], axis=0).astype(jnp.float32)
        up_ext = jnp.concatenate([carried[1], up_pre], axis=0).astype(jnp.float32)
        gate_mix = taps[0, 0] * gate_ext[:-2] + taps[1, 0] * gate_ext[1:-1] + taps[2, 0] * gate_ext[2:]
        up_mix = taps[0, 1] * up_ext[:-2] + taps[1, 1] * up_ext[1:-1] + taps[2, 1] * up_ext[2:]
        hidden = (jax.nn.silu(gate_mix) * up_mix).astype(jnp.bfloat16)
        ffn = jnp.zeros((TOK_DEV, D), jnp.float32)
        for group in range(N_TP):
            part = jnp.dot(hidden[:, group * unit_width:(group + 1) * unit_width], down_projection_weight[:, group * unit_width:(group + 1) * unit_width].T, preferred_element_type=jnp.float32)
            ffn = ffn + lax.optimization_barrier(part.astype(jnp.bfloat16)).astype(jnp.float32)
        layer_block = (stream_block.astype(jnp.float32) + ffn).astype(jnp.bfloat16)
        return ((gate_pre[-2:], up_pre[-2:]), layer_block)
    start_rows = (jnp.zeros((2, FF), jnp.bfloat16), jnp.zeros((2, FF), jnp.bfloat16))
    last_rows, layer_blocks = lax.scan(ffn_block, start_rows, (normed.reshape(block_count, TOK_DEV, D), stream.reshape(block_count, TOK_DEV, D)))
    return layer_blocks.reshape(TOKEN_TOTAL, D)
```

```python
import functools

import jax
import jax.numpy as jnp
from jax import lax
from jax.experimental import pallas as pl
from jax.experimental.pallas import tpu as pltpu
from jax.sharding import PartitionSpec as P

HEAD_WIDTH = 64
BLOCK = 64
PER_STEP = 4
PIECES = 4
MESH = pl.DeviceIdType.MESH
WIDE = jnp.float32
NARROW = jnp.bfloat16


def mul(a, b, dims=((1,), (0,))):
    return lax.dot_general(
        a.astype(NARROW), b.astype(NARROW), (dims, ((), ())), preferred_element_type=WIDE
    )


def parts_of(a, count):
    found = []
    for _ in range(count):
        piece = a.astype(NARROW)
        found.append(piece)
        a = a - piece.astype(WIDE)
    return found


def fine_left(a, b, count, dims=((1,), (0,))):
    return sum(mul(piece, b, dims) for piece in parts_of(a, count))


def fine_right(a, b, count, dims=((1,), (0,))):
    return sum(mul(a, piece, dims) for piece in parts_of(b, count))


def head_mask(width):
    rows = lax.broadcasted_iota(jnp.int32, (width, width), 0) // HEAD_WIDTH
    lanes = lax.broadcasted_iota(jnp.int32, (width, width), 1) // HEAD_WIDTH
    return jnp.where(rows == lanes, 1.0, 0.0)


def stacked(a, mask):
    a = a.astype(NARROW)
    return jnp.concatenate([a] * (mask.shape[0] // a.shape[0]), axis=0) * mask


def fine_product(a, b, mask):
    a_high, a_low = parts_of(a, 2)
    b_high, b_low = (stacked(piece, mask) for piece in parts_of(b, 2))
    return mul(a_high, b_high) + mul(a_low, b_high) + mul(a_high, b_low)


def collapsed(a):
    heads = a.shape[0] // HEAD_WIDTH
    return sum(a[h * HEAD_WIDTH : (h + 1) * HEAD_WIDTH] for h in range(heads))


def recurrence_kernel(
    q_ref, k_ref, v_ref, decay_ref, rate_ref, extra_ref, local_ref, reach_ref, map_ref, state
):
    width = q_ref.shape[1]
    mask_wide = head_mask(width)
    mask = mask_wide.astype(NARROW)
    last = ((1,), (1,))
    first = ((0,), (0,))

    @pl.when(pl.program_id(0) == 0)
    def _():
        rows = lax.broadcasted_iota(jnp.int32, (width, width), 0)
        lanes = lax.broadcasted_iota(jnp.int32, (width, width), 1)
        state[:, :width] = jnp.zeros((width, width), WIDE)
        state[:, width:] = jnp.where(rows == lanes, 1.0, 0.0)

    token = lax.broadcasted_iota(jnp.int32, (BLOCK, width), 0)
    other = lax.broadcasted_iota(jnp.int32, (BLOCK, width), 1) % BLOCK
    strict = token > other
    within = token >= other
    eye = jnp.where(token == other, 1.0, 0.0)
    lower = jnp.where(
        lax.broadcasted_iota(jnp.int32, (BLOCK, BLOCK), 0)
        >= lax.broadcasted_iota(jnp.int32, (BLOCK, BLOCK), 1),
        1.0,
        0.0,
    ).astype(NARROW)
    ones = jnp.ones((BLOCK, width), NARROW)

    prepared = []
    for part in range(PER_STEP):
        at = slice(part * BLOCK, (part + 1) * BLOCK)
        q = q_ref[at].astype(WIDE)
        k = k_ref[at].astype(WIDE)
        v = stacked(v_ref[at], mask)
        log_decay = (
            -jnp.exp(-0.5) * jax.nn.sigmoid(decay_ref[at].astype(WIDE)) + extra_ref[at]
        )
        rates = jax.nn.sigmoid(rate_ref[at].astype(WIDE))
        normed = k * lax.rsqrt(fine_left(k * k, mask, 2) + 1e-06)
        removal = normed * rates
        cum = fine_right(lower, log_decay, 3)
        previous = cum - log_decay
        middle = cum[BLOCK // 2 : BLOCK // 2 + 1]
        end = cum[BLOCK - 1 : BLOCK]
        back = jnp.exp(middle - cum)
        left = jnp.concatenate(
            [normed * jnp.exp(previous - middle), q * jnp.exp(cum - middle)], axis=0
        )
        by_key = mul(left, stacked(k * back, mask), last)
        by_removal = mul(left, stacked(removal * back, mask), last)
        key_rate = jnp.where(strict, by_key[:BLOCK], 0.0)
        removal_rate = jnp.where(strict, by_removal[:BLOCK], 0.0)
        key_out = jnp.where(within, by_key[BLOCK:], 0.0)
        removal_out = jnp.where(within, by_removal[BLOCK:], 0.0)
        inverse = eye
        size = 1
        while size < BLOCK:
            pair = (token // (2 * size) == other // (2 * size)) & (
                token // size != other // size
            )
            piece = jnp.where(pair, removal_rate, 0.0)
            if size == 1:
                inverse = inverse - piece
            else:
                inverse = inverse - fine_product(fine_product(inverse, piece, mask), inverse, mask)
            size *= 2
        from_state = mul(inverse, stacked(normed * jnp.exp(previous), mask))
        keyed = mul(jnp.concatenate([key_rate, key_out], axis=0), v)
        offset = mul(inverse, stacked(keyed[:BLOCK], mask))
        reach = q * jnp.exp(cum) - mul(removal_out, stacked(from_state, mask))
        local = keyed[BLOCK:] - mul(removal_out, stacked(offset, mask))
        to_end = jnp.exp(end - cum)
        span = jnp.exp(fine_left(log_decay, ones, 3, first))
        prepared.append((from_state, offset, reach, local, k * to_end, removal * to_end, span))

    for part in range(PER_STEP):
        at = slice(part * BLOCK, (part + 1) * BLOCK)
        from_state, offset, reach, local, key_end, removal_end, span = prepared[part]
        now = state[...]
        both = mul(jnp.concatenate([from_state, reach], axis=0), now)
        correction = both[:BLOCK, :width] + offset
        local_ref[at] = local + both[BLOCK:, :width]
        reach_ref[at] = both[BLOCK:, width:]
        kept_value = mul(
            jnp.concatenate([key_end, -removal_end], axis=0),
            jnp.concatenate([v_ref[at].astype(WIDE), correction], axis=0),
            first,
        )
        kept_map = mul(-removal_end, both[:BLOCK, width:], first)
        state[:, :width] = now[:, :width] * span + kept_value * mask_wide
        state[:, width:] = now[:, width:] * span + kept_map * mask_wide

    @pl.when(pl.program_id(0) == pl.num_programs(0) - 1)
    def _():
        map_ref[...] = collapsed(state[...]).astype(NARROW)


def recurrence(q, k, v, decay, rate, extra):
    tokens, width = q.shape
    rows = BLOCK * PER_STEP
    spec = pl.BlockSpec((rows, width), lambda i: (i, 0))
    return pl.pallas_call(
        recurrence_kernel,
        grid=(tokens // rows,),
        in_specs=[spec] * 6,
        out_specs=[spec, spec, pl.BlockSpec((HEAD_WIDTH, 2 * width), lambda i: (0, 0))],
        out_shape=[
            jax.ShapeDtypeStruct((tokens, width), WIDE),
            jax.ShapeDtypeStruct((tokens, width), WIDE),
            jax.ShapeDtypeStruct((HEAD_WIDTH, 2 * width), NARROW),
        ],
        scratch_shapes=[pltpu.VMEM((width, 2 * width), WIDE)],
        compiler_params=pltpu.CompilerParams(
            dimension_semantics=("arbitrary",), vmem_limit_bytes=40 * 1024 * 1024
        ),
        cost_estimate=pl.CostEstimate(
            flops=250 * tokens * width * width * 2, bytes_accessed=8 * tokens * width * 2,
            transcendentals=0,
        ),
        name="recurrence",
    )(q, k, v, decay, rate, extra)


def exchange_kernel(axis, x_ref, o_ref, send_sem, recv_sem, local_sem):
    count = lax.axis_size(axis)
    me = lax.axis_index(axis)
    barrier = pltpu.get_barrier_semaphore()
    for step in range(1, count):
        pl.semaphore_signal(
            barrier, inc=1, device_id={axis: lax.rem(me + step, count)}, device_id_type=MESH
        )
    pl.semaphore_wait(barrier, count - 1)
    own = pltpu.make_async_copy(x_ref, o_ref.at[me], local_sem)
    own.start()
    copies = []
    for step in range(1, count):
        copy = pltpu.make_async_remote_copy(
            src_ref=x_ref,
            dst_ref=o_ref.at[me],
            send_sem=send_sem.at[step - 1],
            recv_sem=recv_sem.at[step - 1],
            device_id={axis: lax.rem(me + step, count)},
            device_id_type=MESH,
        )
        copy.start()
        copies.append(copy)
    own.wait()
    for copy in copies:
        copy.wait()


def exchange(x, axis, identity):
    count = lax.axis_size(axis)
    return pl.pallas_call(
        functools.partial(exchange_kernel, axis),
        out_shape=jax.ShapeDtypeStruct((count,) + x.shape, x.dtype),
        in_specs=[pl.BlockSpec(memory_space=pltpu.VMEM)],
        out_specs=pl.BlockSpec(memory_space=pltpu.VMEM),
        scratch_shapes=[
            pltpu.SemaphoreType.DMA((count - 1,)),
            pltpu.SemaphoreType.DMA((count - 1,)),
            pltpu.SemaphoreType.DMA,
        ],
        compiler_params=pltpu.CompilerParams(collective_id=identity, has_side_effects=True),
        name="exchange",
    )(x)


def pieces_of(axis, rows):
    count = lax.axis_size(axis)
    me = lax.axis_index(axis)
    half = count // 2
    pair = me // 2
    side = lax.rem(me, 2)
    step = rows // PIECES

    def device(offset, sibling):
        group = lax.rem(pair + offset + half, half)
        return 2 * group + (1 - side if sibling else side)

    def window(owner, piece):
        return pl.ds(pl.multiple_of(owner * rows + piece * step, step), step)

    return half, device, window, step


def greet(axis):
    count = lax.axis_size(axis)
    me = lax.axis_index(axis)
    barrier = pltpu.get_barrier_semaphore()
    for step in range(1, count):
        pl.semaphore_signal(
            barrier, inc=1, device_id={axis: lax.rem(me + step, count)}, device_id_type=MESH
        )
    pl.semaphore_wait(barrier, count - 1)


def send(axis, source, target, sems, index, device):
    copy = pltpu.make_async_remote_copy(
        src_ref=source,
        dst_ref=target,
        send_sem=sems[0].at[index],
        recv_sem=sems[1].at[index],
        device_id={axis: device},
        device_id_type=MESH,
    )
    copy.start()
    return copy


def summed_pieces(axis, partial, near, leaving, far, near_sems, far_sems, finish):
    rows = near.shape[1]
    half, device, window, step = pieces_of(axis, rows)
    order = list(range(1, half)) + [0]
    near_copies = {}
    for offset in order:
        for piece in range(PIECES):
            near_copies[offset, piece] = send(
                axis,
                partial.at[window(device(offset, True), piece)],
                near.at[offset, pl.ds(piece * step, step)],
                near_sems,
                offset * PIECES + piece,
                device(0, True),
            )
    far_copies = {}
    for piece in range(PIECES):
        at = pl.ds(piece * step, step)
        for offset in range(1, half):
            near_copies[offset, piece].wait_recv()
            mine = partial[window(device(offset, False), piece)].astype(WIDE)
            leaving[offset - 1, at] = (mine + near[offset, at].astype(WIDE)).astype(NARROW)
            far_copies[offset, piece] = send(
                axis,
                leaving.at[offset - 1, at],
                far.at[offset - 1, at],
                far_sems,
                (offset - 1) * PIECES + piece,
                device(offset, False),
            )
    for piece in range(PIECES):
        at = pl.ds(piece * step, step)
        near_copies[0, piece].wait_recv()
        total = partial[window(device(0, False), piece)].astype(WIDE) + near[0, at].astype(WIDE)
        for offset in range(1, half):
            far_copies[offset, piece].wait_recv()
            total = total + far[offset - 1, at].astype(WIDE)
        finish(piece, at, total)
    for copy in list(near_copies.values()) + list(far_copies.values()):
        copy.wait_send()


def stream_kernel(
    axis, partial, residual, gain, stream, whole, near, leaving, far,
    near_send, near_recv, far_send, far_recv, side_send, side_recv, out_send, out_recv,
    pass_send, pass_recv,
):
    greet(axis)
    half, device, window, _ = pieces_of(axis, residual.shape[0])
    side_copies = {}
    out_copies = {}
    pass_copies = {}

    def finish(piece, at, total):
        kept = (residual[at].astype(WIDE) + total).astype(NARROW)
        stream[at] = kept
        kept = kept.astype(WIDE)
        scale = lax.rsqrt(jnp.mean(kept * kept, axis=-1, keepdims=True) + 1e-06)
        own = window(device(0, False), piece)
        whole[own] = (kept * scale * gain[...]).astype(NARROW)
        for offset in range(1, half):
            out_copies[offset, piece] = send(
                axis, whole.at[own], whole.at[own], (out_send, out_recv),
                (offset - 1) * PIECES + piece, device(offset, False),
            )
        side_copies[piece] = send(
            axis, whole.at[own], whole.at[own], (side_send, side_recv), piece, device(0, True)
        )

    summed_pieces(
        axis, partial, near, leaving, far, (near_send, near_recv), (far_send, far_recv), finish
    )
    for piece in range(PIECES):
        for offset in range(1, half):
            out_copies[offset, piece].wait_recv()
            arrived = window(device(-offset, False), piece)
            pass_copies[offset, piece] = send(
                axis, whole.at[arrived], whole.at[arrived], (pass_send, pass_recv),
                (offset - 1) * PIECES + piece, device(0, True),
            )
    for copy in list(out_copies.values()):
        copy.wait_send()
    for copy in list(side_copies.values()) + list(pass_copies.values()):
        copy.wait()


def closing_kernel(
    axis, partial, stream, out, near, leaving, far, near_send, near_recv, far_send, far_recv
):
    greet(axis)

    def finish(piece, at, total):
        out[at] = (stream[at].astype(WIDE) + total).astype(NARROW)

    summed_pieces(
        axis, partial, near, leaving, far, (near_send, near_recv), (far_send, far_recv), finish
    )


def sum_scratch(axis, rows, features):
    half = lax.axis_size(axis) // 2
    dma = pltpu.SemaphoreType.DMA
    others = (half - 1) * PIECES
    return [
        pltpu.VMEM((half, rows, features), NARROW),
        pltpu.VMEM((half - 1, rows, features), NARROW),
        pltpu.VMEM((half - 1, rows, features), NARROW),
        dma((half * PIECES,)),
        dma((half * PIECES,)),
        dma((others,)),
        dma((others,)),
    ]


def streamed(partial, residual, gain, axis, identity):
    rows, features = residual.shape
    dma = pltpu.SemaphoreType.DMA
    others = (lax.axis_size(axis) // 2 - 1) * PIECES
    in_vmem = pl.BlockSpec(memory_space=pltpu.VMEM)
    return pl.pallas_call(
        functools.partial(stream_kernel, axis),
        in_specs=[in_vmem] * 3,
        out_specs=[in_vmem] * 2,
        out_shape=[
            jax.ShapeDtypeStruct((rows, features), NARROW),
            jax.ShapeDtypeStruct(partial.shape, NARROW),
        ],
        scratch_shapes=sum_scratch(axis, rows, features)
        + [dma((PIECES,)), dma((PIECES,))]
        + [dma((others,))] * 4,
        compiler_params=pltpu.CompilerParams(
            collective_id=identity, has_side_effects=True, vmem_limit_bytes=40 * 1024 * 1024
        ),
        name="streamed",
    )(partial, residual, gain[None])


def closed(partial, stream, axis, identity):
    rows, features = stream.shape
    in_vmem = pl.BlockSpec(memory_space=pltpu.VMEM)
    return pl.pallas_call(
        functools.partial(closing_kernel, axis),
        in_specs=[in_vmem] * 2,
        out_specs=in_vmem,
        out_shape=jax.ShapeDtypeStruct((rows, features), NARROW),
        scratch_shapes=sum_scratch(axis, rows, features),
        compiler_params=pltpu.CompilerParams(
            collective_id=identity, has_side_effects=True, vmem_limit_bytes=40 * 1024 * 1024
        ),
        name="closed",
    )(partial, stream)


def project_kernel(local_ref, reach_ref, maps_ref, gain_ref, gate_ref, weight_ref, out_ref, state):
    width = local_ref.shape[1]
    mask = head_mask(width).astype(NARROW)

    @pl.when(pl.program_id(0) == 0)
    def _():
        place = lax.axis_index("sp")

        def one(step, entering):
            maps = maps_ref[step]
            high, low = parts_of(entering, 2)
            after = (
                maps[:, :width].astype(WIDE)
                + mul(maps[:, width:], stacked(high, mask))
                + mul(maps[:, width:], stacked(low, mask))
            )
            return jnp.where(step < place, after, entering)

        state[...] = lax.fori_loop(
            0, maps_ref.shape[0] - 1, one, jnp.zeros((HEAD_WIDTH, width), WIDE)
        )

    readout = local_ref[...] + mul(reach_ref[...], stacked(state[...], mask))
    centered = readout - fine_left(readout, mask, 2) * (1.0 / HEAD_WIDTH)
    variance = fine_left(centered * centered, mask, 2) * (1.0 / HEAD_WIDTH)
    mixed = (
        centered * lax.rsqrt(variance + 0.00064) * gain_ref[...] * gate_ref[...].astype(WIDE)
    )
    out_ref[...] = mul(mixed, weight_ref[...]).astype(NARROW)


def project(local, reach, maps, gain, gate, weight):
    tokens, width = local.shape
    rows = 256
    spec = pl.BlockSpec((rows, width), lambda i: (i, 0))
    features = weight.shape[1]
    return pl.pallas_call(
        project_kernel,
        grid=(tokens // rows,),
        in_specs=[
            spec,
            spec,
            pl.BlockSpec(maps.shape, lambda i: (0, 0, 0)),
            pl.BlockSpec((1, width), lambda i: (0, 0)),
            spec,
            pl.BlockSpec(weight.shape, lambda i: (0, 0)),
        ],
        out_specs=pl.BlockSpec((rows, features), lambda i: (i, 0)),
        out_shape=jax.ShapeDtypeStruct((tokens, features), NARROW),
        scratch_shapes=[pltpu.VMEM((HEAD_WIDTH, width), WIDE)],
        compiler_params=pltpu.CompilerParams(
            dimension_semantics=("arbitrary",), vmem_limit_bytes=40 * 1024 * 1024
        ),
        name="project",
    )(local, reach, maps, gain[None], gate, weight)


def passed_along(x, axis, by):
    count = lax.axis_size(axis)
    pairs = [(i, i + by) for i in range(count) if 0 <= i + by < count]
    return lax.ppermute(x, axis, pairs)


def conv_mix(before_rows, current, taps):
    extended = jnp.concatenate([before_rows, current], axis=0).astype(jnp.float32)
    return taps[0] * extended[:-2] + taps[1] * extended[1:-1] + taps[2] * extended[2:]


def body(
    residual_input_stream,
    receptance,
    key_matrix_all,
    value_matrix_all,
    decay_preactivation,
    learning_rate_preactivation,
    output_gate_all_heads,
    extra_log_decay,
    head_norm_gain,
    output_projection_weight,
    feedforward_norm_gain,
    gate_projection_weight,
    up_projection_weight,
    down_projection_weight,
    convolution_kernel,
):
    full_gate = lax.all_gather(gate_projection_weight, "sp", axis=0, tiled=True)
    full_up = lax.all_gather(up_projection_weight, "sp", axis=0, tiled=True)
    full_down = lax.all_gather(down_projection_weight, "sp", axis=0, tiled=True)
    local, reach, own_map = recurrence(
        receptance,
        key_matrix_all,
        value_matrix_all,
        decay_preactivation,
        learning_rate_preactivation,
        extra_log_decay,
    )
    maps = exchange(own_map, "sp", 1)
    partial = project(
        local, reach, maps, head_norm_gain, output_gate_all_heads, output_projection_weight
    )
    stream, whole_rows = streamed(
        partial, residual_input_stream, feedforward_norm_gain, "tp", 2
    )
    gate_acc = jnp.dot(whole_rows, full_gate, preferred_element_type=jnp.float32)
    up_acc = jnp.dot(whole_rows, full_up, preferred_element_type=jnp.float32)
    gate_pre = gate_acc.astype(jnp.bfloat16)
    up_pre = up_acc.astype(jnp.bfloat16)
    before = passed_along((gate_pre[-2:], up_pre[-2:]), "sp", 1)
    taps = convolution_kernel.astype(jnp.float32)
    gate_mix = conv_mix(before[0], gate_pre, taps[:, 0])
    up_mix = conv_mix(before[1], up_pre, taps[:, 1])
    hidden = (jax.nn.silu(gate_mix) * up_mix).astype(jnp.bfloat16)
    ffn_part = lax.dot_general(
        hidden, full_down, (((1,), (1,)), ((), ())), preferred_element_type=jnp.float32
    ).astype(jnp.bfloat16)
    return closed(ffn_part, stream, "tp", 3)


def solution(mesh):
    in_specs = (
        P(("sp", "tp"), None),
        P("sp", "tp"),
        P("sp", "tp"),
        P("sp", "tp"),
        P("sp", "tp"),
        P("sp", "tp"),
        P("sp", "tp"),
        P("sp", "tp"),
        P("tp"),
        P("tp", None),
        P(),
        P("sp", "tp"),
        P("sp", "tp"),
        P("sp", "tp"),
        P(None, None, "tp"),
    )
    out_specs = P(("sp", "tp"), None)
    return jax.shard_map(body, mesh=mesh, in_specs=in_specs, out_specs=out_specs, check_vma=False)
```

```python
import functools

import jax
import jax.numpy as jnp
from jax import lax
from jax.experimental import pallas as pl
from jax.experimental.pallas import tpu as pltpu
from jax.sharding import PartitionSpec as P

HEAD_WIDTH = 64
BLOCK = 64
PER_STEP = 4
PIECES = 4
MESH = pl.DeviceIdType.MESH
WIDE = jnp.float32
NARROW = jnp.bfloat16


def mul(a, b, dims=((1,), (0,))):
    return lax.dot_general(
        a.astype(NARROW), b.astype(NARROW), (dims, ((), ())), preferred_element_type=WIDE
    )


def parts_of(a, count):
    found = []
    for _ in range(count):
        piece = a.astype(NARROW)
        found.append(piece)
        a = a - piece.astype(WIDE)
    return found


def fine_left(a, b, count, dims=((1,), (0,))):
    return sum(mul(piece, b, dims) for piece in parts_of(a, count))


def fine_right(a, b, count, dims=((1,), (0,))):
    return sum(mul(a, piece, dims) for piece in parts_of(b, count))


def head_mask(width):
    rows = lax.broadcasted_iota(jnp.int32, (width, width), 0) // HEAD_WIDTH
    lanes = lax.broadcasted_iota(jnp.int32, (width, width), 1) // HEAD_WIDTH
    return jnp.where(rows == lanes, 1.0, 0.0)


def stacked(a, mask):
    a = a.astype(NARROW)
    return jnp.concatenate([a] * (mask.shape[0] // a.shape[0]), axis=0) * mask


def fine_product(a, b, mask):
    a_high, a_low = parts_of(a, 2)
    b_high, b_low = (stacked(piece, mask) for piece in parts_of(b, 2))
    return mul(a_high, b_high) + mul(a_low, b_high) + mul(a_high, b_low)


def collapsed(a):
    heads = a.shape[0] // HEAD_WIDTH
    return sum(a[h * HEAD_WIDTH : (h + 1) * HEAD_WIDTH] for h in range(heads))


def recurrence_kernel(
    q_ref, k_ref, v_ref, decay_ref, rate_ref, extra_ref, local_ref, reach_ref, map_ref, state
):
    width = q_ref.shape[1]
    mask_wide = head_mask(width)
    mask = mask_wide.astype(NARROW)
    last = ((1,), (1,))
    first = ((0,), (0,))

    @pl.when(pl.program_id(0) == 0)
    def _():
        rows = lax.broadcasted_iota(jnp.int32, (width, width), 0)
        lanes = lax.broadcasted_iota(jnp.int32, (width, width), 1)
        state[:, :width] = jnp.zeros((width, width), WIDE)
        state[:, width:] = jnp.where(rows == lanes, 1.0, 0.0)

    token = lax.broadcasted_iota(jnp.int32, (BLOCK, width), 0)
    other = lax.broadcasted_iota(jnp.int32, (BLOCK, width), 1) % BLOCK
    strict = token > other
    within = token >= other
    eye = jnp.where(token == other, 1.0, 0.0)
    lower = jnp.where(
        lax.broadcasted_iota(jnp.int32, (BLOCK, BLOCK), 0)
        >= lax.broadcasted_iota(jnp.int32, (BLOCK, BLOCK), 1),
        1.0,
        0.0,
    ).astype(NARROW)
    ones = jnp.ones((BLOCK, width), NARROW)

    prepared = []
    for part in range(PER_STEP):
        at = slice(part * BLOCK, (part + 1) * BLOCK)
        q = q_ref[at].astype(WIDE)
        k = k_ref[at].astype(WIDE)
        v = stacked(v_ref[at], mask)
        log_decay = (
            -jnp.exp(-0.5) * jax.nn.sigmoid(decay_ref[at].astype(WIDE)) + extra_ref[at]
        )
        rates = jax.nn.sigmoid(rate_ref[at].astype(WIDE))
        normed = k * lax.rsqrt(fine_left(k * k, mask, 2) + 1e-06)
        removal = normed * rates
        cum = fine_right(lower, log_decay, 3)
        previous = cum - log_decay
        middle = cum[BLOCK // 2 : BLOCK // 2 + 1]
        end = cum[BLOCK - 1 : BLOCK]
        back = jnp.exp(middle - cum)
        left = jnp.concatenate(
            [normed * jnp.exp(previous - middle), q * jnp.exp(cum - middle)], axis=0
        )
        by_key = mul(left, stacked(k * back, mask), last)
        by_removal = mul(left, stacked(removal * back, mask), last)
        key_rate = jnp.where(strict, by_key[:BLOCK], 0.0)
        removal_rate = jnp.where(strict, by_removal[:BLOCK], 0.0)
        key_out = jnp.where(within, by_key[BLOCK:], 0.0)
        removal_out = jnp.where(within, by_removal[BLOCK:], 0.0)
        inverse = eye
        size = 1
        while size < BLOCK:
            pair = (token // (2 * size) == other // (2 * size)) & (
                token // size != other // size
            )
            piece = jnp.where(pair, removal_rate, 0.0)
            if size == 1:
                inverse = inverse - piece
            else:
                inverse = inverse - fine_product(fine_product(inverse, piece, mask), inverse, mask)
            size *= 2
        from_state = mul(inverse, stacked(normed * jnp.exp(previous), mask))
        keyed = mul(jnp.concatenate([key_rate, key_out], axis=0), v)
        offset = mul(inverse, stacked(keyed[:BLOCK], mask))
        reach = q * jnp.exp(cum) - mul(removal_out, stacked(from_state, mask))
        local = keyed[BLOCK:] - mul(removal_out, stacked(offset, mask))
        to_end = jnp.exp(end - cum)
        span = jnp.exp(fine_left(log_decay, ones, 3, first))
        prepared.append((from_state, offset, reach, local, k * to_end, removal * to_end, span))

    for part in range(PER_STEP):
        at = slice(part * BLOCK, (part + 1) * BLOCK)
        from_state, offset, reach, local, key_end, removal_end, span = prepared[part]
        now = state[...]
        both = mul(jnp.concatenate([from_state, reach], axis=0), now)
        correction = both[:BLOCK, :width] + offset
        local_ref[at] = local + both[BLOCK:, :width]
        reach_ref[at] = both[BLOCK:, width:]
        kept_value = mul(
            jnp.concatenate([key_end, -removal_end], axis=0),
            jnp.concatenate([v_ref[at].astype(WIDE), correction], axis=0),
            first,
        )
        kept_map = mul(-removal_end, both[:BLOCK, width:], first)
        state[:, :width] = now[:, :width] * span + kept_value * mask_wide
        state[:, width:] = now[:, width:] * span + kept_map * mask_wide

    @pl.when(pl.program_id(0) == pl.num_programs(0) - 1)
    def _():
        map_ref[...] = collapsed(state[...]).astype(NARROW)


def recurrence(q, k, v, decay, rate, extra):
    tokens, width = q.shape
    rows = BLOCK * PER_STEP
    spec = pl.BlockSpec((rows, width), lambda i: (i, 0))
    return pl.pallas_call(
        recurrence_kernel,
        grid=(tokens // rows,),
        in_specs=[spec] * 6,
        out_specs=[spec, spec, pl.BlockSpec((HEAD_WIDTH, 2 * width), lambda i: (0, 0))],
        out_shape=[
            jax.ShapeDtypeStruct((tokens, width), WIDE),
            jax.ShapeDtypeStruct((tokens, width), WIDE),
            jax.ShapeDtypeStruct((HEAD_WIDTH, 2 * width), NARROW),
        ],
        scratch_shapes=[pltpu.VMEM((width, 2 * width), WIDE)],
        compiler_params=pltpu.CompilerParams(
            dimension_semantics=("arbitrary",), vmem_limit_bytes=40 * 1024 * 1024
        ),
        cost_estimate=pl.CostEstimate(
            flops=250 * tokens * width * width * 2, bytes_accessed=8 * tokens * width * 2,
            transcendentals=0,
        ),
        name="recurrence",
    )(q, k, v, decay, rate, extra)


def exchange_kernel(axis, x_ref, o_ref, send_sem, recv_sem, local_sem):
    count = lax.axis_size(axis)
    me = lax.axis_index(axis)
    barrier = pltpu.get_barrier_semaphore()
    for step in range(1, count):
        pl.semaphore_signal(
            barrier, inc=1, device_id={axis: lax.rem(me + step, count)}, device_id_type=MESH
        )
    pl.semaphore_wait(barrier, count - 1)
    own = pltpu.make_async_copy(x_ref, o_ref.at[me], local_sem)
    own.start()
    copies = []
    for step in range(1, count):
        copy = pltpu.make_async_remote_copy(
            src_ref=x_ref,
            dst_ref=o_ref.at[me],
            send_sem=send_sem.at[step - 1],
            recv_sem=recv_sem.at[step - 1],
            device_id={axis: lax.rem(me + step, count)},
            device_id_type=MESH,
        )
        copy.start()
        copies.append(copy)
    own.wait()
    for copy in copies:
        copy.wait()


def exchange(x, axis, identity):
    count = lax.axis_size(axis)
    return pl.pallas_call(
        functools.partial(exchange_kernel, axis),
        out_shape=jax.ShapeDtypeStruct((count,) + x.shape, x.dtype),
        in_specs=[pl.BlockSpec(memory_space=pltpu.VMEM)],
        out_specs=pl.BlockSpec(memory_space=pltpu.VMEM),
        scratch_shapes=[
            pltpu.SemaphoreType.DMA((count - 1,)),
            pltpu.SemaphoreType.DMA((count - 1,)),
            pltpu.SemaphoreType.DMA,
        ],
        compiler_params=pltpu.CompilerParams(collective_id=identity, has_side_effects=True),
        name="exchange",
    )(x)


def pieces_of(axis, rows):
    count = lax.axis_size(axis)
    me = lax.axis_index(axis)
    half = count // 2
    pair = me // 2
    side = lax.rem(me, 2)
    step = rows // PIECES

    def device(offset, sibling):
        group = lax.rem(pair + offset + half, half)
        return 2 * group + (1 - side if sibling else side)

    def window(owner, piece):
        return pl.ds(pl.multiple_of(owner * rows + piece * step, step), step)

    return half, device, window, step


def greet(axis, more=0):
    count = lax.axis_size(axis)
    me = lax.axis_index(axis)
    barrier = pltpu.get_barrier_semaphore()
    for step in range(1, count):
        pl.semaphore_signal(
            barrier, inc=1, device_id={axis: lax.rem(me + step, count)}, device_id_type=MESH
        )
    pl.semaphore_wait(barrier, count - 1 + more)


def send(axis, source, target, sems, index, device):
    copy = pltpu.make_async_remote_copy(
        src_ref=source,
        dst_ref=target,
        send_sem=sems[0].at[index],
        recv_sem=sems[1].at[index],
        device_id={axis: device},
        device_id_type=MESH,
    )
    copy.start()
    return copy


def summed_pieces(axis, partial, near, leaving, far, near_sems, far_sems, finish, between=None):
    rows = near.shape[1]
    half, device, window, step = pieces_of(axis, rows)
    order = list(range(1, half)) + [0]
    near_copies = {}
    for offset in order:
        for piece in range(PIECES):
            near_copies[offset, piece] = send(
                axis,
                partial.at[window(device(offset, True), piece)],
                near.at[offset, pl.ds(piece * step, step)],
                near_sems,
                offset * PIECES + piece,
                device(0, True),
            )
    far_copies = {}
    for piece in range(PIECES):
        at = pl.ds(piece * step, step)
        for offset in range(1, half):
            near_copies[offset, piece].wait_recv()
            mine = partial[window(device(offset, False), piece)].astype(WIDE)
            leaving[offset - 1, at] = (mine + near[offset, at].astype(WIDE)).astype(NARROW)
            far_copies[offset, piece] = send(
                axis,
                leaving.at[offset - 1, at],
                far.at[offset - 1, at],
                far_sems,
                (offset - 1) * PIECES + piece,
                device(offset, False),
            )
    if between is not None:
        between()
    for piece in range(PIECES):
        at = pl.ds(piece * step, step)
        near_copies[0, piece].wait_recv()
        total = partial[window(device(0, False), piece)].astype(WIDE) + near[0, at].astype(WIDE)
        for offset in range(1, half):
            far_copies[offset, piece].wait_recv()
            total = total + far[offset - 1, at].astype(WIDE)
        finish(piece, at, total)
    for copy in list(near_copies.values()) + list(far_copies.values()):
        copy.wait_send()


class Ring:
    def __init__(self, axis, shard, gathered, sems, local_sem):
        self.axis, self.shard, self.gathered, self.sems = axis, shard, gathered, sems
        self.count = lax.axis_size(axis)
        me = lax.axis_index(axis)
        odd = lax.rem(me, 2)
        self.place = (1 - odd) * (me // 2) + odd * (self.count - 1 - me // 2)
        self.ahead = self.count // 2
        self.behind = self.count - 1 - self.ahead
        self.hop = 0
        self.going = {}
        self.sent = []
        self.own = pltpu.make_async_copy(shard, self.block(0), local_sem)

    def index(self, offset):
        at = lax.rem(self.place + offset + 2 * self.count, self.count)
        upper = at // (self.count // 2)
        return (1 - upper) * 2 * at + upper * (2 * (self.count - 1 - at) + 1)

    def block(self, offset):
        rows = self.shard.shape[0]
        return self.gathered.at[pl.ds(pl.multiple_of(self.index(offset) * rows, rows), rows)]

    def move(self):
        for copy in self.going.values():
            copy.wait_recv()
            self.sent.append(copy)
        self.going = {}
        for way, limit, base in ((1, self.ahead, 0), (-1, self.behind, self.ahead)):
            if self.hop < limit:
                source = self.shard if self.hop == 0 else self.block(-way * self.hop)
                self.going[way] = send(
                    self.axis, source, self.block(-way * self.hop), self.sems,
                    base + self.hop, self.index(way),
                )
        self.hop += 1

    def finish(self):
        while self.going:
            self.move()
        for copy in self.sent:
            copy.wait_send()
        self.own.wait()


def stream_kernel(
    axis, ring_axis, partial, residual, gain, shard, stream, whole, gathered,
    near, leaving, far,
    near_send, near_recv, far_send, far_recv, side_send, side_recv, out_send, out_recv,
    pass_send, pass_recv, ring_send, ring_recv, own_sem,
):
    ring = Ring(ring_axis, shard, gathered, (ring_send, ring_recv), own_sem)
    barrier = pltpu.get_barrier_semaphore()
    for way in (1, -1):
        pl.semaphore_signal(
            barrier, inc=1, device_id={ring_axis: ring.index(way)}, device_id_type=MESH
        )
    greet(axis, 2)
    ring.own.start()
    ring.move()
    half, device, window, _ = pieces_of(axis, residual.shape[0])
    side_copies = {}
    out_copies = {}
    pass_copies = {}

    def finish(piece, at, total):
        kept = (residual[at].astype(WIDE) + total).astype(NARROW)
        stream[at] = kept
        kept = kept.astype(WIDE)
        scale = lax.rsqrt(jnp.mean(kept * kept, axis=-1, keepdims=True) + 1e-06)
        own = window(device(0, False), piece)
        whole[own] = (kept * scale * gain[...]).astype(NARROW)
        for offset in range(1, half):
            out_copies[offset, piece] = send(
                axis, whole.at[own], whole.at[own], (out_send, out_recv),
                (offset - 1) * PIECES + piece, device(offset, False),
            )
        side_copies[piece] = send(
            axis, whole.at[own], whole.at[own], (side_send, side_recv), piece, device(0, True)
        )

    summed_pieces(
        axis, partial, near, leaving, far, (near_send, near_recv), (far_send, far_recv), finish,
        ring.move,
    )
    ring.move()
    for piece in range(PIECES):
        for offset in range(1, half):
            out_copies[offset, piece].wait_recv()
            arrived = window(device(-offset, False), piece)
            pass_copies[offset, piece] = send(
                axis, whole.at[arrived], whole.at[arrived], (pass_send, pass_recv),
                (offset - 1) * PIECES + piece, device(0, True),
            )
    ring.finish()
    for copy in list(out_copies.values()):
        copy.wait_send()
    for copy in list(side_copies.values()) + list(pass_copies.values()):
        copy.wait()


def closing_kernel(
    axis, partial, stream, out, near, leaving, far, near_send, near_recv, far_send, far_recv
):
    greet(axis)

    def finish(piece, at, total):
        out[at] = (stream[at].astype(WIDE) + total).astype(NARROW)

    summed_pieces(
        axis, partial, near, leaving, far, (near_send, near_recv), (far_send, far_recv), finish
    )


def sum_scratch(axis, rows, features):
    half = lax.axis_size(axis) // 2
    dma = pltpu.SemaphoreType.DMA
    others = (half - 1) * PIECES
    return [
        pltpu.VMEM((half, rows, features), NARROW),
        pltpu.VMEM((half - 1, rows, features), NARROW),
        pltpu.VMEM((half - 1, rows, features), NARROW),
        dma((half * PIECES,)),
        dma((half * PIECES,)),
        dma((others,)),
        dma((others,)),
    ]


def streamed(partial, residual, gain, shard, axis, ring, identity):
    around = lax.axis_size(ring)
    hops = around - 1
    rows, features = residual.shape
    dma = pltpu.SemaphoreType.DMA
    others = (lax.axis_size(axis) // 2 - 1) * PIECES
    in_vmem = pl.BlockSpec(memory_space=pltpu.VMEM)
    return pl.pallas_call(
        functools.partial(stream_kernel, axis, ring),
        in_specs=[in_vmem] * 4,
        out_specs=[in_vmem] * 2 + [pl.BlockSpec(memory_space=pl.ANY)],
        out_shape=[
            jax.ShapeDtypeStruct((rows, features), NARROW),
            jax.ShapeDtypeStruct(partial.shape, NARROW),
            jax.ShapeDtypeStruct((around * shard.shape[0], shard.shape[1]), NARROW),
        ],
        scratch_shapes=sum_scratch(axis, rows, features)
        + [dma((PIECES,)), dma((PIECES,))]
        + [dma((others,))] * 4
        + [dma((hops,)), dma((hops,)), dma],
        compiler_params=pltpu.CompilerParams(
            collective_id=identity, has_side_effects=True, vmem_limit_bytes=40 * 1024 * 1024
        ),
        name="streamed",
    )(partial, residual, gain[None], shard)


def closed(partial, stream, axis, identity):
    rows, features = stream.shape
    in_vmem = pl.BlockSpec(memory_space=pltpu.VMEM)
    return pl.pallas_call(
        functools.partial(closing_kernel, axis),
        in_specs=[in_vmem] * 2,
        out_specs=in_vmem,
        out_shape=jax.ShapeDtypeStruct((rows, features), NARROW),
        scratch_shapes=sum_scratch(axis, rows, features),
        compiler_params=pltpu.CompilerParams(
            collective_id=identity, has_side_effects=True, vmem_limit_bytes=40 * 1024 * 1024
        ),
        name="closed",
    )(partial, stream)


def project_kernel(local_ref, reach_ref, maps_ref, gain_ref, gate_ref, weight_ref, out_ref, state):
    width = local_ref.shape[1]
    mask = head_mask(width).astype(NARROW)

    @pl.when(pl.program_id(0) == 0)
    def _():
        place = lax.axis_index("sp")

        def one(step, entering):
            maps = maps_ref[step]
            high, low = parts_of(entering, 2)
            after = (
                maps[:, :width].astype(WIDE)
                + mul(maps[:, width:], stacked(high, mask))
                + mul(maps[:, width:], stacked(low, mask))
            )
            return jnp.where(step < place, after, entering)

        state[...] = lax.fori_loop(
            0, maps_ref.shape[0] - 1, one, jnp.zeros((HEAD_WIDTH, width), WIDE)
        )

    readout = local_ref[...] + mul(reach_ref[...], stacked(state[...], mask))
    centered = readout - fine_left(readout, mask, 2) * (1.0 / HEAD_WIDTH)
    variance = fine_left(centered * centered, mask, 2) * (1.0 / HEAD_WIDTH)
    mixed = (
        centered * lax.rsqrt(variance + 0.00064) * gain_ref[...] * gate_ref[...].astype(WIDE)
    )
    out_ref[...] = mul(mixed, weight_ref[...]).astype(NARROW)


def project(local, reach, maps, gain, gate, weight):
    tokens, width = local.shape
    rows = 256
    spec = pl.BlockSpec((rows, width), lambda i: (i, 0))
    features = weight.shape[1]
    return pl.pallas_call(
        project_kernel,
        grid=(tokens // rows,),
        in_specs=[
            spec,
            spec,
            pl.BlockSpec(maps.shape, lambda i: (0, 0, 0)),
            pl.BlockSpec((1, width), lambda i: (0, 0)),
            spec,
            pl.BlockSpec(weight.shape, lambda i: (0, 0)),
        ],
        out_specs=pl.BlockSpec((rows, features), lambda i: (i, 0)),
        out_shape=jax.ShapeDtypeStruct((tokens, features), NARROW),
        scratch_shapes=[pltpu.VMEM((HEAD_WIDTH, width), WIDE)],
        compiler_params=pltpu.CompilerParams(
            dimension_semantics=("arbitrary",), vmem_limit_bytes=40 * 1024 * 1024
        ),
        name="project",
    )(local, reach, maps, gain[None], gate, weight)


def passed_along(x, axis, by):
    count = lax.axis_size(axis)
    pairs = [(i, i + by) for i in range(count) if 0 <= i + by < count]
    return lax.ppermute(x, axis, pairs)


def conv_mix(before_rows, current, taps):
    extended = jnp.concatenate([before_rows, current], axis=0).astype(jnp.float32)
    return taps[0] * extended[:-2] + taps[1] * extended[1:-1] + taps[2] * extended[2:]


def body(
    residual_input_stream,
    receptance,
    key_matrix_all,
    value_matrix_all,
    decay_preactivation,
    learning_rate_preactivation,
    output_gate_all_heads,
    extra_log_decay,
    head_norm_gain,
    output_projection_weight,
    feedforward_norm_gain,
    gate_projection_weight,
    up_projection_weight,
    down_projection_weight,
    convolution_kernel,
):
    full_gate = lax.all_gather(gate_projection_weight, "sp", axis=0, tiled=True)
    full_up = lax.all_gather(up_projection_weight, "sp", axis=0, tiled=True)
    local, reach, own_map = recurrence(
        receptance,
        key_matrix_all,
        value_matrix_all,
        decay_preactivation,
        learning_rate_preactivation,
        extra_log_decay,
    )
    maps = exchange(own_map, "sp", 1)
    partial = project(
        local, reach, maps, head_norm_gain, output_gate_all_heads, output_projection_weight
    )
    stream, whole_rows, full_down = streamed(
        partial,
        residual_input_stream,
        feedforward_norm_gain,
        down_projection_weight,
        "tp",
        "sp",
        2,
    )
    gate_acc = jnp.dot(whole_rows, full_gate, preferred_element_type=jnp.float32)
    up_acc = jnp.dot(whole_rows, full_up, preferred_element_type=jnp.float32)
    gate_pre = gate_acc.astype(jnp.bfloat16)
    up_pre = up_acc.astype(jnp.bfloat16)
    before = passed_along((gate_pre[-2:], up_pre[-2:]), "sp", 1)
    taps = convolution_kernel.astype(jnp.float32)
    gate_mix = conv_mix(before[0], gate_pre, taps[:, 0])
    up_mix = conv_mix(before[1], up_pre, taps[:, 1])
    hidden = (jax.nn.silu(gate_mix) * up_mix).astype(jnp.bfloat16)
    ffn_part = lax.dot_general(
        hidden, full_down, (((1,), (1,)), ((), ())), preferred_element_type=jnp.float32
    ).astype(jnp.bfloat16)
    return closed(ffn_part, stream, "tp", 3)


def solution(mesh):
    in_specs = (
        P(("sp", "tp"), None),
        P("sp", "tp"),
        P("sp", "tp"),
        P("sp", "tp"),
        P("sp", "tp"),
        P("sp", "tp"),
        P("sp", "tp"),
        P("sp", "tp"),
        P("tp"),
        P("tp", None),
        P(),
        P("sp", "tp"),
        P("sp", "tp"),
        P("sp", "tp"),
        P(None, None, "tp"),
    )
    out_specs = P(("sp", "tp"), None)
    return jax.shard_map(body, mesh=mesh, in_specs=in_specs, out_specs=out_specs, check_vma=False)
```
